32 devices in a mesh: fs: 8 (over z, x), tp: 4 (over y, core).
Axes of the slice: x: 2, y: 2, z: 4, core: 2. Of those that a mesh axis runs over, the one named last changes fastest.
Arguments:
- tokens: bfloat16 [8192, 2048], P('fs', 'tp'), may hold values from -50 to 50
- norm_gain: float32 [2048], P('fs'), may hold values from 0.1 to 1.9
- gate_weight: float32 [2048, 2816], P('fs', 'tp'), may hold values from -0.125 to 0.125
- up_weight: float32 [2048, 2816], P('fs', 'tp'), may hold values from -0.125 to 0.125
- down_weight: float32 [2816, 2048], P('fs', 'tp'), may hold values from -0.109375 to 0.109375
Outputs:
- gate_sampler: bfloat16 [2048, 2816], P(None, 'tp')
- up_sampler: bfloat16 [2048, 2816], P(None, 'tp')
- down_sampler: bfloat16 [2816, 2048], P('tp')
- mixed: bfloat16 [8192, 2048], P('fs', 'tp')
The draws below stay inside these ranges and needn't reach their ends.
All inputs are finite; a program needn't handle non-finite values.
Results may differ from the reference program's by a relative error of at most 0.0095.
Values may be sent and summed in bfloat16 or wider, within the bound.
A program may use at most 128 MiB of HBM per device.

```python
import math
import jax
import jax.numpy as jnp
from jax import lax

D = 2048
FF = 2816
TOKENS = 8192
HID_DEV = 704
N_TP = 4


def draw_tokens(key, part):
    first, second, third = jax.random.split(key, 3)
    row_scale = jnp.exp(jax.random.uniform(first, (TOKENS, 1), jnp.float32, 0.0, math.log(10.0)))
    col_scale = jnp.exp(jax.random.uniform(second, (1, D), jnp.float32, 0.0, math.log(10.0)))
    base = jnp.clip(jax.random.normal(third, (TOKENS, D), jnp.float32), -5.0, 5.0)
    return (base * row_scale * col_scale / 10.0).astype(jnp.bfloat16)


def steps_of(key, shape, cuts, low, high):
    gain, own = 1.0, jax.random.fold_in(key, 6)
    for axis_at, shards_of in cuts:
        steps = jnp.exp(jax.random.uniform(jax.random.fold_in(own, axis_at), (shards_of,), jnp.float32, low / len(cuts), high / len(cuts)))
        gain = gain * jnp.repeat(steps, shape[axis_at] // shards_of).reshape([-1 if axis == axis_at else 1 for axis in range(len(shape))])
    return gain


def gaussian(rng, shape, scale, limit, cuts=(), held_as=jnp.bfloat16):
    factor_of = steps_of(rng, shape, cuts, -0.22, 0.18) if cuts else 1.0
    values = jax.random.normal(rng, shape, jnp.float32) * scale * factor_of
    return jnp.minimum(jnp.maximum(values, -limit), limit).astype(held_as)


def setup_inputs(seed: int = 0) -> dict:
    key_of = jax.random.split(jax.random.key(seed), 6)
    return {
        "tokens": draw_tokens(jax.random.fold_in(key_of[5], 71), 0),
        "norm_gain": jnp.clip(1.0 + 0.18 * jax.random.normal(key_of[1], (D,), jnp.float32), 0.1, 1.9),
        "gate_weight": gaussian(key_of[2], (D, FF), D ** -0.5, 0.125, ((0, 8), (1, 4)), jnp.float32),
        "up_weight": gaussian(key_of[3], (D, FF), D ** -0.5, 0.125, ((0, 8), (1, 4)), jnp.float32),
        "down_weight": gaussian(key_of[4], (FF, D), FF ** -0.5, 0.109375, ((0, 8), (1, 4)), jnp.float32),
    }


norm_eps = 1e-06

def reference(tokens, norm_gain, gate_weight, up_weight, down_weight):
    gate_sampler = (norm_gain[:, None] * gate_weight).astype(jnp.bfloat16)
    up_sampler = (norm_gain[:, None] * up_weight).astype(jnp.bfloat16)
    down_sampler = down_weight.astype(jnp.bfloat16)
    floated = tokens.astype(jnp.float32)
    normed = (floated * lax.rsqrt(lax.optimization_barrier(jnp.mean(floated * floated, axis=-1, keepdims=True)) + norm_eps)).astype(jnp.bfloat16)
    gate = jnp.dot(normed, gate_sampler, preferred_element_type=jnp.float32)
    up = jnp.dot(normed, up_sampler, preferred_element_type=jnp.float32)
    hidden = (jax.nn.silu(gate) * up).astype(jnp.bfloat16)
    summed = jnp.zeros((tokens.shape[0], tokens.shape[1]), jnp.float32)
    for block_index in range(N_TP):
        low = block_index * HID_DEV
        partial_value = jnp.dot(hidden[:, low:low + HID_DEV], down_sampler[low:low + HID_DEV, :], preferred_element_type=jnp.float32).astype(jnp.bfloat16)
        partial_value = lax.optimization_barrier(partial_value)
        summed = summed + partial_value.astype(jnp.float32)
    return (gate_sampler, up_sampler, down_sampler, summed.astype(jnp.bfloat16))
```

```python
import functools

import jax
import jax.numpy as jnp
from jax import lax
from jax.experimental import pallas as pl
from jax.experimental.pallas import tpu as pltpu
from jax.sharding import PartitionSpec as P

norm_eps = 1e-06
MESH = pl.DeviceIdType.MESH
PIECES = 2
NT = (((1,), (1,)), ((), ()))


def remote(src, dst, send, recv, device):
    return pltpu.make_async_remote_copy(
        src_ref=src, dst_ref=dst, send_sem=send, recv_sem=recv, device_id=device, device_id_type=MESH
    )


def layer_kernel(
    lines, tp,
    tok_in, gate_in, up_in, down_in,
    gate_out, up_out, down_out, mixed_out,
    tok, normed, gu, hidden, down, part, got,
    gu_recv, gu_line, gu_pair, down_recv, down_line, down_pair, down_first,
    tok_recv, tok_send, sum_recv, sum_send, local, stored,
):
    f, t = lax.axis_index("fs"), lax.axis_index("tp")
    z, x = f // 2, f % 2
    sibling = t + 1 - 2 * (t % 2)
    across = (t + 2) % 4
    gu_in, gu_out = (gate_in, up_in), (gate_out, up_out)
    depth = gate_in.shape[1]
    down_rows, width = down_in.shape
    n_tok = tok_in.shape[0]
    tile = n_tok // tp
    pair_dev = {"fs": 2 * z + 1 - x}
    away = jnp.maximum(z - t, t - z)

    def column(k):
        return 2 * ((t // 2 + 1 - k // 2) % 2) + (t % 2 + 1 - k % 2) % 2

    barrier = pltpu.get_barrier_semaphore()
    for other in range(1, tp):
        pl.semaphore_signal(barrier, inc=1, device_id={"tp": (t + other) % tp}, device_id_type=MESH)
    pl.semaphore_signal(barrier, inc=1, device_id=pair_dev, device_id_type=MESH)

    @pl.when(z > 0)
    def _():
        pl.semaphore_signal(barrier, inc=1, device_id={"fs": f - 2}, device_id_type=MESH)

    @pl.when(z < lines - 1)
    def _():
        pl.semaphore_signal(barrier, inc=1, device_id={"fs": f + 2}, device_id_type=MESH)

    pl.semaphore_wait(barrier, tp + jnp.minimum(z, 1) + jnp.minimum(lines - 1 - z, 1))

    def gu_slot(block, p):
        return gu.at[block, p]

    def gu_source(step, block, p):
        return gu_in[p] if step == 0 else gu_slot(block, p)

    def line_copy(step, p, up):
        block = 2 * (z - step if up else z + step) + x
        return remote(
            gu_source(step, block, p), gu_slot(block, p), gu_line.at[0 if up else 1, step, p],
            gu_recv.at[block, p], {"fs": f + 2 if up else f - 2},
        )

    def pair_copy(step, level, p):
        block = 2 * level + x
        return remote(gu_source(step, block, p), gu_slot(block, p), gu_pair.at[level, p], gu_recv.at[block, p], pair_dev)

    def gu_arrived(block, p):
        remote(gu_slot(block, p), gu_slot(block, p), gu_pair.at[0, 0], gu_recv.at[block, p], pair_dev).wait_recv()

    def down_slot(c, j):
        return down.at[c, pl.ds(pl.multiple_of(j * down_rows, down_rows), down_rows)]

    def down_line_copy(c, up):
        return remote(
            down_slot(c, x), down_slot(c, x), down_line.at[0 if up else 1, c], down_recv.at[x, c],
            {"fs": f + 2 if up else f - 2},
        )

    def down_pair_copy(c):
        return remote(down_slot(c, x), down_slot(c, x), down_pair.at[c], down_recv.at[x, c], pair_dev)

    def down_arrived(c, j):
        remote(down_slot(c, j), down_slot(c, j), down_first, down_recv.at[j, c], pair_dev).wait_recv()

    first_copy = remote(down_in, down_slot(t, x), down_first, down_recv.at[x, t], {"tp": z})
    own_gate = pltpu.make_async_copy(gate_in, gu_slot(f, 0), local.at[0])
    own_up = pltpu.make_async_copy(up_in, gu_slot(f, 1), local.at[3])
    own_tok = pltpu.make_async_copy(tok_in, tok.at[t], local.at[1])
    own_down = pltpu.make_async_copy(down_in, down_slot(t, x), local.at[2])
    tok_near = remote(tok_in, tok.at[t], tok_send.at[0], tok_recv.at[t], {"tp": sibling})
    tok_far = remote(tok_in, tok.at[t], tok_send.at[1], tok_recv.at[t], {"tp": across})
    tok_relay = remote(tok.at[across], tok.at[across], tok_send.at[2], tok_recv.at[across], {"tp": sibling})

    def tok_arrived(s):
        remote(tok.at[s], tok.at[s], tok_send.at[0], tok_recv.at[s], {"tp": sibling}).wait_recv()

    def each_line(step, act):
        for p in range(PIECES):
            for up in (True, False):
                level = z - step if up else z + step

                @pl.when((level >= 0) & (level < lines))
                def _():
                    if act == "start" and step > 0:
                        gu_arrived(2 * level + x, p)

                    @pl.when(z < lines - 1 if up else z > 0)
                    def _():
                        copy = line_copy(step, p, up)
                        copy.start() if act == "start" else copy.wait_send()

                    if step > 0 or up:
                        copy = pair_copy(step, level, p)
                        copy.start() if act == "start" else copy.wait_send()

    def each_down(step, act):
        for k in range(tp):
            c = column(k)

            @pl.when(away == step)
            def _():
                if act == "start":
                    if step == 0:
                        @pl.when(c != t)
                        def _():
                            down_arrived(c, x)
                    else:
                        down_arrived(c, x)

                for up in (True, False):
                    @pl.when((z >= t) & (z < lines - 1) if up else (z <= t) & (z > 0))
                    def _():
                        copy = down_line_copy(c, up)
                        copy.start() if act == "start" else copy.wait_send()

    each_line(0, "start")

    @pl.when(t != z)
    def _():
        first_copy.start()

    tok_far.start()
    tok_near.start()
    own_gate.start()
    own_up.start()
    own_tok.start()

    @pl.when(t == z)
    def _():
        own_down.start()
        own_down.wait()

    for step in range(1, lines):
        each_line(step, "start")
        each_down(step - 1, "start")
        if step == lines // 2:
            tok_arrived(across)
            tok_relay.start()

    @pl.when(away < lines - 1)
    def _():
        for k in range(tp):
            down_pair_copy(column(k)).start()

    own_tok.wait()
    tok_arrived(sibling)
    tok_arrived(3 - t)
    norm_tile = min(128, n_tok)

    def norm_rows(i, carry):
        at = pl.ds(pl.multiple_of(i * norm_tile, norm_tile), norm_tile)
        total = jnp.zeros((norm_tile, 1), jnp.float32)
        for s in range(tp):
            value = tok[s, at, :].astype(jnp.float32)
            total = total + jnp.sum(value * value, axis=-1, keepdims=True)
        scale = lax.rsqrt(total / (tp * width) + norm_eps)
        for s in range(tp):
            normed[at, s * width:(s + 1) * width] = (tok[s, at, :].astype(jnp.float32) * scale).astype(jnp.bfloat16)
        return carry

    lax.fori_loop(0, n_tok // norm_tile, norm_rows, 0)

    own_gate.wait()
    own_up.wait()
    for level in range(lines):
        for p in range(PIECES):
            gu_arrived(2 * level + 1 - x, p)

    def gu_store(block, p):
        return pltpu.make_async_copy(
            gu_slot(block, p), gu_out[p].at[:, block * depth:(block + 1) * depth], stored.at[block, p]
        )

    for block in range(2 * lines):
        for p in range(PIECES):
            gu_store(block, p).start()

    def hidden_rows(i, carry):
        at = pl.ds(pl.multiple_of(i * tile, tile), tile)
        value = normed[at, :]
        gate, up = (
            lax.dot_general(
                value, jnp.concatenate([gu[block, p] for block in range(2 * lines)], axis=1), NT,
                preferred_element_type=jnp.float32,
            )
            for p in range(PIECES)
        )
        hidden[at, :] = (gate / (1.0 + jnp.exp(-gate)) * up).astype(jnp.bfloat16)

        @pl.when(away == lines - 1)
        def _():
            c = column(i)
            down_arrived(c, x)
            down_pair_copy(c).start()

        return carry

    lax.fori_loop(0, tp, hidden_rows, 0)

    def down_store(k):
        c = column(k)
        return pltpu.make_async_copy(
            down.at[c], down_out.at[:, pl.ds(pl.multiple_of(c * width, width), width)], local.at[4 + k]
        )

    sends = [
        remote(part.at[0], got.at[0], sum_send.at[0], sum_recv.at[0], {"tp": sibling}),
        remote(part.at[1], got.at[1], sum_send.at[1], sum_recv.at[1], {"tp": across}),
        remote(part.at[2], got.at[2], sum_send.at[2], sum_recv.at[2], {"tp": sibling}),
    ]
    for k in range(tp):
        c = column(k)
        down_arrived(c, 1 - x)
        down_store(k).start()
        if k == 1:
            sends[0].wait_recv()
        if k == 3:
            sends[2].wait_recv()
            sends[1].wait_recv()

        def part_rows(i, carry):
            at = pl.ds(pl.multiple_of(i * tile, tile), tile)
            value = jnp.dot(hidden[at, :], down[c], preferred_element_type=jnp.float32)
            if k == 1:
                value = value + got[0, at, :].astype(jnp.float32)
            if k == 3:
                value = value + got[2, at, :].astype(jnp.float32) + got[1, at, :].astype(jnp.float32)
                mixed_out[at, :] = value.astype(jnp.bfloat16)
            else:
                part[k, at, :] = value.astype(jnp.bfloat16)
            return carry

        lax.fori_loop(0, tp, part_rows, 0)
        if k < 3:
            sends[k].start()

    for step in range(lines):
        each_line(step, "wait")
    for step in range(lines - 1):
        each_down(step, "wait")
    for k in range(tp):
        down_pair_copy(column(k)).wait_send()
        down_store(k).wait()

    @pl.when(t != z)
    def _():
        first_copy.wait_send()

    tok_near.wait_send()
    tok_far.wait_send()
    tok_relay.wait_send()
    for copy in sends:
        copy.wait_send()
    for block in range(2 * lines):
        for p in range(PIECES):
            gu_store(block, p).wait()


def fused(fs, tp, tokens, gate_local, up_local, down_local):
    lines = fs // 2
    n_tok, width = tokens.shape
    depth, units = gate_local.shape
    down_rows = down_local.shape[0]
    bf16 = jnp.bfloat16
    dma = pltpu.SemaphoreType.DMA
    vmem = pl.BlockSpec(memory_space=pltpu.VMEM)
    anywhere = pl.BlockSpec(memory_space=pl.ANY)
    gate, up, down_sampler, mixed = pl.pallas_call(
        functools.partial(layer_kernel, lines, tp),
        out_shape=(
            jax.ShapeDtypeStruct((units, fs * depth), bf16),
            jax.ShapeDtypeStruct((units, fs * depth), bf16),
            jax.ShapeDtypeStruct((2 * down_rows, tp * width), bf16),
            jax.ShapeDtypeStruct((n_tok, width), bf16),
        ),
        in_specs=[vmem] * 4,
        out_specs=(anywhere, anywhere, anywhere, vmem),
        scratch_shapes=[
            pltpu.VMEM((tp, n_tok, width), bf16),
            pltpu.VMEM((n_tok, tp * width), bf16),
            pltpu.VMEM((fs, PIECES, units, depth), bf16),
            pltpu.VMEM((n_tok, units), bf16),
            pltpu.VMEM((tp, 2 * down_rows, width), bf16),
            pltpu.VMEM((3, n_tok, width), bf16),
            pltpu.VMEM((3, n_tok, width), bf16),
            dma((fs, PIECES)), dma((2, lines, PIECES)), dma((lines, PIECES)),
            dma((2, tp)), dma((2, tp)), dma((tp,)), dma,
            dma((tp,)), dma((3,)), dma((3,)), dma((3,)), dma((4 + tp,)), dma((fs, PIECES)),
        ],
        compiler_params=pltpu.CompilerParams(
            collective_id=0, has_side_effects=True, vmem_limit_bytes=56 * 1024 * 1024
        ),
    )(tokens, gate_local.T, up_local.T, down_local)
    return gate.T, up.T, down_sampler, mixed


def plain(tokens, gate_local, up_local, down_local):
    gathered = lax.all_gather(tokens, "tp", axis=1, tiled=True)
    floated = gathered.astype(jnp.float32)
    normed = (
        floated * lax.rsqrt(jnp.mean(floated * floated, axis=-1, keepdims=True) + norm_eps)
    ).astype(jnp.bfloat16)
    gate_sampler = lax.all_gather(gate_local, "fs", axis=0, tiled=True)
    up_sampler = lax.all_gather(up_local, "fs", axis=0, tiled=True)
    gate = jnp.dot(normed, gate_sampler, preferred_element_type=jnp.float32)
    up = jnp.dot(normed, up_sampler, preferred_element_type=jnp.float32)
    hidden = (jax.nn.silu(gate) * up).astype(jnp.bfloat16)
    down_columns = lax.all_gather(down_local, "fs", axis=0, tiled=True)
    down_sampler = lax.all_to_all(down_columns, "tp", split_axis=0, concat_axis=1, tiled=True)
    mixed = jnp.dot(
        lax.all_gather(hidden, "tp", axis=1, tiled=True), down_columns, preferred_element_type=jnp.float32
    ).astype(jnp.bfloat16)
    return gate_sampler, up_sampler, down_sampler, mixed


def shards(fs, tp, tokens, norm_gain, gate_weight, up_weight, down_weight):
    gate_local = (norm_gain[:, None] * gate_weight).astype(jnp.bfloat16)
    up_local = (norm_gain[:, None] * up_weight).astype(jnp.bfloat16)
    down_local = down_weight.astype(jnp.bfloat16)
    aligned = (
        gate_local.shape[0] % 128 == 0
        and gate_local.shape[1] % 16 == 0
        and down_local.shape[0] % 16 == 0
        and down_local.shape[1] % 128 == 0
        and tokens.shape[0] % (128 * tp) == 0
    )
    if not (tp == 4 and fs == 2 * tp and aligned):
        return plain(tokens, gate_local, up_local, down_local)
    return fused(fs, tp, tokens, gate_local, up_local, down_local)


def solution(mesh):
    return jax.shard_map(
        functools.partial(shards, mesh.shape["fs"], mesh.shape["tp"]),
        mesh=mesh,
        in_specs=(P("fs", "tp"), P("fs"), P("fs", "tp"), P("fs", "tp"), P("fs", "tp")),
        out_specs=(P(None, "tp"), P(None, "tp"), P("tp", None), P("fs", "tp")),
        check_vma=False,
    )
```

```python
import functools

import jax
import jax.numpy as jnp
from jax import lax
from jax.experimental import pallas as pl
from jax.experimental.pallas import tpu as pltpu
from jax.sharding import PartitionSpec as P

norm_eps = 1e-06
MESH = pl.DeviceIdType.MESH
PIECES = 2
NT = (((1,), (1,)), ((), ()))
WHOLE = 1


def remote(src, dst, send, recv, device):
    return pltpu.make_async_remote_copy(
        src_ref=src, dst_ref=dst, send_sem=send, recv_sem=recv, device_id=device, device_id_type=MESH
    )


def layer_kernel(
    lines, tp,
    tok_in, gate_in, up_in, down_in,
    gate_out, up_out, down_out, mixed_out,
    tok, normed, gu, hidden, down, part, got,
    gu_recv, gu_line, gu_pair, down_recv, down_line, down_pair, down_first,
    tok_recv, tok_send, sum_recv, sum_send, local, stored,
):
    f, t = lax.axis_index("fs"), lax.axis_index("tp")
    z, x = f // 2, f % 2
    sibling = t + 1 - 2 * (t % 2)
    across = (t + 2) % 4
    gu_in, gu_out = (gate_in, up_in), (gate_out, up_out)
    depth = gate_in.shape[1]
    down_rows, width = down_in.shape
    n_tok = tok_in.shape[0]
    tile = n_tok // tp
    pair_dev = {"fs": 2 * z + 1 - x}
    away = jnp.maximum(z - t, t - z)

    def column(k):
        return 2 * ((t // 2 + 1 - k // 2) % 2) + (t % 2 + 1 - k % 2) % 2

    barrier = pltpu.get_barrier_semaphore()
    for other in range(1, tp):
        pl.semaphore_signal(barrier, inc=1, device_id={"tp": (t + other) % tp}, device_id_type=MESH)
    pl.semaphore_signal(barrier, inc=1, device_id=pair_dev, device_id_type=MESH)

    @pl.when(z > 0)
    def _():
        pl.semaphore_signal(barrier, inc=1, device_id={"fs": f - 2}, device_id_type=MESH)

    @pl.when(z < lines - 1)
    def _():
        pl.semaphore_signal(barrier, inc=1, device_id={"fs": f + 2}, device_id_type=MESH)

    pl.semaphore_wait(barrier, tp + jnp.minimum(z, 1) + jnp.minimum(lines - 1 - z, 1))

    def gu_slot(block, p):
        return gu.at[block, p]

    def gu_source(step, block, p):
        return gu_in[p] if step == 0 else gu_slot(block, p)

    def line_copy(step, p, up):
        block = 2 * (z - step if up else z + step) + x
        return remote(
            gu_source(step, block, p), gu_slot(block, p), gu_line.at[0 if up else 1, step, p],
            gu_recv.at[block, p], {"fs": f + 2 if up else f - 2},
        )

    def pair_copy(step, level, p):
        block = 2 * level + x
        return remote(gu_source(step, block, p), gu_slot(block, p), gu_pair.at[level, p], gu_recv.at[block, p], pair_dev)

    def gu_arrived(block, p):
        remote(gu_slot(block, p), gu_slot(block, p), gu_pair.at[0, 0], gu_recv.at[block, p], pair_dev).wait_recv()

    def down_slot(c, j):
        return down.at[c, pl.ds(pl.multiple_of(j * down_rows, down_rows), down_rows)]

    def down_line_copy(c, j, up):
        return remote(
            down_slot(c, j), down_slot(c, j), down_line.at[0 if up else 1, j, c], down_recv.at[j, c],
            {"fs": f + 2 if up else f - 2},
        )

    def down_pair_copy(c):
        return remote(down_slot(c, x), down_slot(c, x), down_pair.at[c], down_recv.at[x, c], pair_dev)

    def down_arrived(c, j):
        remote(down_slot(c, j), down_slot(c, j), down_first, down_recv.at[j, c], pair_dev).wait_recv()

    first_copy = remote(down_in, down_slot(t, x), down_first, down_recv.at[x, t], {"tp": z})
    own_gate = pltpu.make_async_copy(gate_in, gu_slot(f, 0), local.at[0])
    own_up = pltpu.make_async_copy(up_in, gu_slot(f, 1), local.at[3])
    own_tok = pltpu.make_async_copy(tok_in, tok.at[t], local.at[1])
    own_down = pltpu.make_async_copy(down_in, down_slot(t, x), local.at[2])
    tok_near = remote(tok_in, tok.at[t], tok_send.at[0], tok_recv.at[t], {"tp": sibling})
    tok_far = remote(tok_in, tok.at[t], tok_send.at[1], tok_recv.at[t], {"tp": across})
    tok_relay = remote(tok.at[across], tok.at[across], tok_send.at[2], tok_recv.at[across], {"tp": sibling})

    def tok_arrived(s):
        remote(tok.at[s], tok.at[s], tok_send.at[0], tok_recv.at[s], {"tp": sibling}).wait_recv()

    def each_line(step, act):
        for p in range(PIECES):
            for up in (True, False):
                level = z - step if up else z + step

                @pl.when((level >= 0) & (level < lines))
                def _():
                    if act == "start" and step > 0:
                        gu_arrived(2 * level + x, p)

                    @pl.when(z < lines - 1 if up else z > 0)
                    def _():
                        copy = line_copy(step, p, up)
                        copy.start() if act == "start" else copy.wait_send()

                    if step > 0 or up:
                        copy = pair_copy(step, level, p)
                        copy.start() if act == "start" else copy.wait_send()

    def each_down(step, act):
        for k in (WHOLE,) + tuple(k for k in range(tp) if k != WHOLE):
            c = column(k)

            @pl.when(away == step)
            def _():
                if act == "start":
                    if step == 0 and k != WHOLE:
                        @pl.when(c != t)
                        def _():
                            down_arrived(c, x)
                    if step > 0:
                        down_arrived(c, x)
                    if k == WHOLE:
                        down_arrived(c, 1 - x)

                for up in (True, False):
                    @pl.when((z >= t) & (z < lines - 1) if up else (z <= t) & (z > 0))
                    def _():
                        for j in (x, 1 - x) if k == WHOLE else (x,):
                            copy = down_line_copy(c, j, up)
                            copy.start() if act == "start" else copy.wait_send()

    each_line(0, "start")

    @pl.when(t != z)
    def _():
        first_copy.start()

    tok_far.start()
    tok_near.start()
    own_gate.start()
    own_up.start()
    own_tok.start()

    @pl.when(t == z)
    def _():
        own_down.start()
        own_down.wait()

    @pl.when(t == z)
    def _():
        down_arrived(column(WHOLE), x)
        down_pair_copy(column(WHOLE)).start()

    for step in range(1, lines):
        each_line(step, "start")
        if step > 1:
            each_down(step - 2, "start")
        if step == lines // 2:
            tok_arrived(across)
            tok_relay.start()

    each_down(lines - 2, "start")

    @pl.when(away < lines - 1)
    def _():
        for k in range(tp):
            if k != WHOLE:
                down_pair_copy(column(k)).start()

    own_tok.wait()
    tok_arrived(sibling)
    tok_arrived(3 - t)
    norm_tile = min(128, n_tok)

    def norm_rows(i, carry):
        at = pl.ds(pl.multiple_of(i * norm_tile, norm_tile), norm_tile)
        total = jnp.zeros((norm_tile, 1), jnp.float32)
        for s in range(tp):
            value = tok[s, at, :].astype(jnp.float32)
            total = total + jnp.sum(value * value, axis=-1, keepdims=True)
        scale = lax.rsqrt(total / (tp * width) + norm_eps)
        for s in range(tp):
            normed[at, s * width:(s + 1) * width] = (tok[s, at, :].astype(jnp.float32) * scale).astype(jnp.bfloat16)
        return carry

    lax.fori_loop(0, n_tok // norm_tile, norm_rows, 0)

    own_gate.wait()
    own_up.wait()
    for level in range(lines):
        for p in range(PIECES):
            gu_arrived(2 * level + 1 - x, p)

    def gu_store(block, p):
        return pltpu.make_async_copy(
            gu_slot(block, p), gu_out[p].at[:, block * depth:(block + 1) * depth], stored.at[block, p]
        )

    for block in range(2 * lines):
        for p in range(PIECES):
            gu_store(block, p).start()

    def hidden_rows(i, carry):
        at = pl.ds(pl.multiple_of(i * tile, tile), tile)
        value = normed[at, :]
        gate, up = (
            lax.dot_general(
                value, jnp.concatenate([gu[block, p] for block in range(2 * lines)], axis=1), NT,
                preferred_element_type=jnp.float32,
            )
            for p in range(PIECES)
        )
        hidden[at, :] = (gate / (1.0 + jnp.exp(-gate)) * up).astype(jnp.bfloat16)

        @pl.when(away == lines - 1)
        def _():
            c = column(i)
            down_arrived(c, x)

            @pl.when(i == WHOLE)
            def _():
                down_arrived(c, 1 - x)

            @pl.when(i != WHOLE)
            def _():
                down_pair_copy(c).start()

        return carry

    lax.fori_loop(0, tp, hidden_rows, 0)

    def down_store(k):
        c = column(k)
        return pltpu.make_async_copy(
            down.at[c], down_out.at[:, pl.ds(pl.multiple_of(c * width, width), width)], local.at[4 + k]
        )

    sends = [
        remote(part.at[0], got.at[0], sum_send.at[0], sum_recv.at[0], {"tp": sibling}),
        remote(part.at[1], got.at[1], sum_send.at[1], sum_recv.at[1], {"tp": across}),
        remote(part.at[2], got.at[2], sum_send.at[2], sum_recv.at[2], {"tp": sibling}),
    ]
    for k in range(tp):
        c = column(k)
        if k != WHOLE:
            down_arrived(c, 1 - x)
        down_store(k).start()
        if k == 1:
            sends[0].wait_recv()
        if k == 3:
            sends[2].wait_recv()
            sends[1].wait_recv()

        def part_rows(i, carry):
            at = pl.ds(pl.multiple_of(i * tile, tile), tile)
            value = jnp.dot(hidden[at, :], down[c], preferred_element_type=jnp.float32)
            if k == 1:
                value = value + got[0, at, :].astype(jnp.float32)
            if k == 3:
                value = value + got[2, at, :].astype(jnp.float32) + got[1, at, :].astype(jnp.float32)
                mixed_out[at, :] = value.astype(jnp.bfloat16)
            else:
                part[k, at, :] = value.astype(jnp.bfloat16)
            return carry

        lax.fori_loop(0, tp, part_rows, 0)
        if k < 3:
            sends[k].start()

    for step in range(lines):
        each_line(step, "wait")
    for step in range(lines - 1):
        each_down(step, "wait")
    for k in range(tp):
        if k != WHOLE:
            down_pair_copy(column(k)).wait_send()
        down_store(k).wait()

    @pl.when(t == z)
    def _():
        down_pair_copy(column(WHOLE)).wait_send()

    @pl.when(t != z)
    def _():
        first_copy.wait_send()

    tok_near.wait_send()
    tok_far.wait_send()
    tok_relay.wait_send()
    for copy in sends:
        copy.wait_send()
    for block in range(2 * lines):
        for p in range(PIECES):
            gu_store(block, p).wait()


def fused(fs, tp, tokens, gate_local, up_local, down_local):
    lines = fs // 2
    n_tok, width = tokens.shape
    depth, units = gate_local.shape
    down_rows = down_local.shape[0]
    bf16 = jnp.bfloat16
    dma = pltpu.SemaphoreType.DMA
    vmem = pl.BlockSpec(memory_space=pltpu.VMEM)
    anywhere = pl.BlockSpec(memory_space=pl.ANY)
    gate, up, down_sampler, mixed = pl.pallas_call(
        functools.partial(layer_kernel, lines, tp),
        out_shape=(
            jax.ShapeDtypeStruct((units, fs * depth), bf16),
            jax.ShapeDtypeStruct((units, fs * depth), bf16),
            jax.ShapeDtypeStruct((2 * down_rows, tp * width), bf16),
            jax.ShapeDtypeStruct((n_tok, width), bf16),
        ),
        in_specs=[vmem] * 4,
        out_specs=(anywhere, anywhere, anywhere, vmem),
        scratch_shapes=[
            pltpu.VMEM((tp, n_tok, width), bf16),
            pltpu.VMEM((n_tok, tp * width), bf16),
            pltpu.VMEM((fs, PIECES, units, depth), bf16),
            pltpu.VMEM((n_tok, units), bf16),
            pltpu.VMEM((tp, 2 * down_rows, width), bf16),
            pltpu.VMEM((3, n_tok, width), bf16),
            pltpu.VMEM((3, n_tok, width), bf16),
            dma((fs, PIECES)), dma((2, lines, PIECES)), dma((lines, PIECES)),
            dma((2, tp)), dma((2, 2, tp)), dma((tp,)), dma,
            dma((tp,)), dma((3,)), dma((3,)), dma((3,)), dma((4 + tp,)), dma((fs, PIECES)),
        ],
        compiler_params=pltpu.CompilerParams(
            collective_id=0, has_side_effects=True, vmem_limit_bytes=40 * 1024 * 1024
        ),
    )(tokens, gate_local.T, up_local.T, down_local)
    return gate.T, up.T, down_sampler, mixed


def plain(tokens, gate_local, up_local, down_local):
    gathered = lax.all_gather(tokens, "tp", axis=1, tiled=True)
    floated = gathered.astype(jnp.float32)
    normed = (
        floated * lax.rsqrt(jnp.mean(floated * floated, axis=-1, keepdims=True) + norm_eps)
    ).astype(jnp.bfloat16)
    gate_sampler = lax.all_gather(gate_local, "fs", axis=0, tiled=True)
    up_sampler = lax.all_gather(up_local, "fs", axis=0, tiled=True)
    gate = jnp.dot(normed, gate_sampler, preferred_element_type=jnp.float32)
    up = jnp.dot(normed, up_sampler, preferred_element_type=jnp.float32)
    hidden = (jax.nn.silu(gate) * up).astype(jnp.bfloat16)
    down_columns = lax.all_gather(down_local, "fs", axis=0, tiled=True)
    down_sampler = lax.all_to_all(down_columns, "tp", split_axis=0, concat_axis=1, tiled=True)
    mixed = jnp.dot(
        lax.all_gather(hidden, "tp", axis=1, tiled=True), down_columns, preferred_element_type=jnp.float32
    ).astype(jnp.bfloat16)
    return gate_sampler, up_sampler, down_sampler, mixed


def shards(fs, tp, tokens, norm_gain, gate_weight, up_weight, down_weight):
    gate_local = (norm_gain[:, None] * gate_weight).astype(jnp.bfloat16)
    up_local = (norm_gain[:, None] * up_weight).astype(jnp.bfloat16)
    down_local = down_weight.astype(jnp.bfloat16)
    aligned = (
        gate_local.shape[0] % 128 == 0
        and gate_local.shape[1] % 16 == 0
        and down_local.shape[0] % 16 == 0
        and down_local.shape[1] % 128 == 0
        and tokens.shape[0] % (128 * tp) == 0
    )
    if not (tp == 4 and fs == 2 * tp and aligned):
        return plain(tokens, gate_local, up_local, down_local)
    return fused(fs, tp, tokens, gate_local, up_local, down_local)


def solution(mesh):
    return jax.shard_map(
        functools.partial(shards, mesh.shape["fs"], mesh.shape["tp"]),
        mesh=mesh,
        in_specs=(P("fs", "tp"), P("fs"), P("fs", "tp"), P("fs", "tp"), P("fs", "tp")),
        out_specs=(P(None, "tp"), P(None, "tp"), P("tp", None), P("fs", "tp")),
        check_vma=False,
    )
```

```python
import functools

import jax
import jax.numpy as jnp
from jax import lax
from jax.experimental import pallas as pl
from jax.experimental.pallas import tpu as pltpu
from jax.sharding import PartitionSpec as P

norm_eps = 1e-06
MESH = pl.DeviceIdType.MESH
PIECES = 2
NT = (((1,), (1,)), ((), ()))
WHOLE = 1


def remote(src, dst, send, recv, device):
    return pltpu.make_async_remote_copy(
        src_ref=src, dst_ref=dst, send_sem=send, recv_sem=recv, device_id=device, device_id_type=MESH
    )


def layer_kernel(
    lines, tp,
    tok_in, gate_in, up_in, down_in,
    gate_out, up_out, down_out, mixed_out,
    tok, normed, gu, hidden, down, part, got,
    gu_recv, gu_line, gu_pair, down_recv, down_line, down_pair, down_first,
    tok_recv, tok_send, sum_recv, sum_send, local, stored,
):
    f, t = lax.axis_index("fs"), lax.axis_index("tp")
    z, x = f // 2, f % 2
    sibling = t + 1 - 2 * (t % 2)
    across = (t + 2) % 4
    gu_in, gu_out = (gate_in, up_in), (gate_out, up_out)
    depth = gate_in.shape[1]
    down_rows, width = down_in.shape
    n_tok = tok_in.shape[0]
    tile = n_tok // tp
    pair_dev = {"fs": 2 * z + 1 - x}
    away = jnp.maximum(z - t, t - z)

    def column(k):
        return 2 * ((t // 2 + 1 - k // 2) % 2) + (t % 2 + 1 - k % 2) % 2

    barrier = pltpu.get_barrier_semaphore()
    for other in range(1, tp):
        pl.semaphore_signal(barrier, inc=1, device_id={"tp": (t + other) % tp}, device_id_type=MESH)
    pl.semaphore_signal(barrier, inc=1, device_id=pair_dev, device_id_type=MESH)

    @pl.when(z > 0)
    def _():
        pl.semaphore_signal(barrier, inc=1, device_id={"fs": f - 2}, device_id_type=MESH)

    @pl.when(z < lines - 1)
    def _():
        pl.semaphore_signal(barrier, inc=1, device_id={"fs": f + 2}, device_id_type=MESH)

    pl.semaphore_wait(barrier, tp + jnp.minimum(z, 1) + jnp.minimum(lines - 1 - z, 1))

    def gu_slot(block, p):
        return gu.at[block, p]

    def gu_source(step, block, p):
        return gu_in[p] if step == 0 else gu_slot(block, p)

    def line_copy(step, p, up):
        block = 2 * (z - step if up else z + step) + x
        return remote(
            gu_source(step, block, p), gu_slot(block, p), gu_line.at[0 if up else 1, step, p],
            gu_recv.at[block, p], {"fs": f + 2 if up else f - 2},
        )

    def pair_copy(step, level, p):
        block = 2 * level + x
        return remote(gu_source(step, block, p), gu_slot(block, p), gu_pair.at[level, p], gu_recv.at[block, p], pair_dev)

    def gu_arrived(block, p):
        remote(gu_slot(block, p), gu_slot(block, p), gu_pair.at[0, 0], gu_recv.at[block, p], pair_dev).wait_recv()

    def down_slot(c, j):
        return down.at[c, pl.ds(pl.multiple_of(j * down_rows, down_rows), down_rows)]

    def down_line_copy(c, j, up):
        return remote(
            down_slot(c, j), down_slot(c, j), down_line.at[0 if up else 1, j, c], down_recv.at[j, c],
            {"fs": f + 2 if up else f - 2},
        )

    def down_pair_copy(c):
        return remote(down_slot(c, x), down_slot(c, x), down_pair.at[c], down_recv.at[x, c], pair_dev)

    def down_arrived(c, j):
        remote(down_slot(c, j), down_slot(c, j), down_first, down_recv.at[j, c], pair_dev).wait_recv()

    first_copy = remote(down_in, down_slot(t, x), down_first, down_recv.at[x, t], {"tp": z})
    own_gate = pltpu.make_async_copy(gate_in, gu_slot(f, 0), local.at[0])
    own_up = pltpu.make_async_copy(up_in, gu_slot(f, 1), local.at[3])
    own_tok = pltpu.make_async_copy(tok_in, tok.at[t], local.at[1])
    own_down = pltpu.make_async_copy(down_in, down_slot(t, x), local.at[2])
    tok_near = remote(tok_in, tok.at[t], tok_send.at[0], tok_recv.at[t], {"tp": sibling})
    tok_far = remote(tok_in, tok.at[t], tok_send.at[1], tok_recv.at[t], {"tp": across})
    tok_relay = remote(tok.at[across], tok.at[across], tok_send.at[2], tok_recv.at[across], {"tp": sibling})

    def tok_arrived(s):
        remote(tok.at[s], tok.at[s], tok_send.at[0], tok_recv.at[s], {"tp": sibling}).wait_recv()

    def each_line(step, act):
        for p in range(PIECES):
            for up in (True, False):
                level = z - step if up else z + step

                @pl.when((level >= 0) & (level < lines))
                def _():
                    if act == "start" and step > 0:
                        gu_arrived(2 * level + x, p)

                    @pl.when(z < lines - 1 if up else z > 0)
                    def _():
                        copy = line_copy(step, p, up)
                        copy.start() if act == "start" else copy.wait_send()

                    if step > 0 or up:
                        copy = pair_copy(step, level, p)
                        copy.start() if act == "start" else copy.wait_send()

    def each_down(step, act):
        for k in (WHOLE,) + tuple(k for k in range(tp) if k != WHOLE):
            c = column(k)

            @pl.when(away == step)
            def _():
                if act == "start":
                    if step == 0 and k != WHOLE:
                        @pl.when(c != t)
                        def _():
                            down_arrived(c, x)
                    if step > 0:
                        down_arrived(c, x)
                    if k == WHOLE:
                        down_arrived(c, 1 - x)

                for up in (True, False):
                    @pl.when((z >= t) & (z < lines - 1) if up else (z <= t) & (z > 0))
                    def _():
                        for j in (x, 1 - x) if k == WHOLE else (x,):
                            copy = down_line_copy(c, j, up)
                            copy.start() if act == "start" else copy.wait_send()

    each_line(0, "start")

    @pl.when(t != z)
    def _():
        first_copy.start()

    tok_far.start()
    tok_near.start()
    own_gate.start()
    own_up.start()
    own_tok.start()

    @pl.when(t == z)
    def _():
        own_down.start()
        own_down.wait()

    @pl.when(t == z)
    def _():
        down_arrived(column(WHOLE), x)
        down_pair_copy(column(WHOLE)).start()

    for step in range(1, lines):
        each_line(step, "start")
        if step > 1:
            each_down(step - 2, "start")
        if step == lines // 2:
            tok_arrived(across)
            tok_relay.start()

    each_down(lines - 2, "start")

    @pl.when(away < lines - 1)
    def _():
        for k in range(tp):
            if k != WHOLE:
                down_pair_copy(column(k)).start()

    own_tok.wait()
    tok_arrived(sibling)
    tok_arrived(3 - t)
    norm_tile = min(128, n_tok)

    def norm_rows(i, carry):
        at = pl.ds(pl.multiple_of(i * norm_tile, norm_tile), norm_tile)
        total = jnp.zeros((norm_tile, 1), jnp.float32)
        for s in range(tp):
            value = tok[s, at, :].astype(jnp.float32)
            total = total + jnp.sum(value * value, axis=-1, keepdims=True)
        scale = lax.rsqrt(total / (tp * width) + norm_eps)
        for s in range(tp):
            normed[at, s * width:(s + 1) * width] = (tok[s, at, :].astype(jnp.float32) * scale).astype(jnp.bfloat16)
        return carry

    lax.fori_loop(0, n_tok // norm_tile, norm_rows, 0)

    own_gate.wait()
    own_up.wait()
    for level in range(lines):
        for p in range(PIECES):
            gu_arrived(2 * level + 1 - x, p)

    def gu_store(block, p):
        return pltpu.make_async_copy(
            gu_slot(block, p), gu_out[p].at[:, block * depth:(block + 1) * depth], stored.at[block, p]
        )

    for block in range(2 * lines):
        for p in range(PIECES):
            gu_store(block, p).start()

    def down_store(k):
        c = column(k)
        return pltpu.make_async_copy(
            down.at[c], down_out.at[:, pl.ds(pl.multiple_of(c * width, width), width)], local.at[4 + k]
        )

    def tile_rows(i):
        return pl.ds(pl.multiple_of(i * tile, tile), tile)

    def sum_copy(k, i):
        at = tile_rows(i)
        return remote(
            part.at[k, at], got.at[k, at], sum_send.at[k, i], sum_recv.at[k, i], {"tp": across if k == 1 else sibling}
        )

    def partial(k, at):
        return jnp.dot(hidden[at, :], down[column(k)], preferred_element_type=jnp.float32)

    def first_rows(i, carry):
        at = tile_rows(i)
        value = normed[at, :]
        gate, up = (
            lax.dot_general(
                value, jnp.concatenate([gu[block, p] for block in range(2 * lines)], axis=1), NT,
                preferred_element_type=jnp.float32,
            )
            for p in range(PIECES)
        )
        hidden[at, :] = (gate / (1.0 + jnp.exp(-gate)) * up).astype(jnp.bfloat16)

        @pl.when(away == lines - 1)
        def _():
            @pl.when(i != WHOLE)
            def _():
                down_arrived(column(i), x)
                down_pair_copy(column(i)).start()

            @pl.when(i == 0)
            def _():
                down_arrived(column(WHOLE), x)
                down_arrived(column(WHOLE), 1 - x)

        @pl.when(i == 0)
        def _():
            down_arrived(column(0), 1 - x)
            down_store(0).start()
            down_store(1).start()

        part[0, at, :] = partial(0, at).astype(jnp.bfloat16)
        value = partial(1, at)
        sum_copy(0, i).start()
        sum_copy(0, i).wait_recv()
        part[1, at, :] = (value + got[0, at, :].astype(jnp.float32)).astype(jnp.bfloat16)
        sum_copy(1, i).start()
        return carry

    lax.fori_loop(0, tp, first_rows, 0)
    down_arrived(column(2), 1 - x)
    down_store(2).start()

    def near_rows(i, carry):
        at = tile_rows(i)
        part[2, at, :] = partial(2, at).astype(jnp.bfloat16)
        sum_copy(2, i).start()
        return carry

    lax.fori_loop(0, tp, near_rows, 0)
    down_arrived(column(3), 1 - x)
    down_store(3).start()

    def last_rows(i, carry):
        at = tile_rows(i)
        value = partial(3, at)
        sum_copy(2, i).wait_recv()
        sum_copy(1, i).wait_recv()
        value = value + got[2, at, :].astype(jnp.float32) + got[1, at, :].astype(jnp.float32)
        mixed_out[at, :] = value.astype(jnp.bfloat16)
        return carry

    lax.fori_loop(0, tp, last_rows, 0)

    for step in range(lines):
        each_line(step, "wait")
    for step in range(lines - 1):
        each_down(step, "wait")
    for k in range(tp):
        if k != WHOLE:
            down_pair_copy(column(k)).wait_send()
        down_store(k).wait()

    @pl.when(t == z)
    def _():
        down_pair_copy(column(WHOLE)).wait_send()

    @pl.when(t != z)
    def _():
        first_copy.wait_send()

    tok_near.wait_send()
    tok_far.wait_send()
    tok_relay.wait_send()
    for k in range(3):
        for i in range(tp):
            sum_copy(k, i).wait_send()
    for block in range(2 * lines):
        for p in range(PIECES):
            gu_store(block, p).wait()


def fused(fs, tp, tokens, gate_local, up_local, down_local):
    lines = fs // 2
    n_tok, width = tokens.shape
    depth, units = gate_local.shape
    down_rows = down_local.shape[0]
    bf16 = jnp.bfloat16
    dma = pltpu.SemaphoreType.DMA
    vmem = pl.BlockSpec(memory_space=pltpu.VMEM)
    anywhere = pl.BlockSpec(memory_space=pl.ANY)
    gate, up, down_sampler, mixed = pl.pallas_call(
        functools.partial(layer_kernel, lines, tp),
        out_shape=(
            jax.ShapeDtypeStruct((units, fs * depth), bf16),
            jax.ShapeDtypeStruct((units, fs * depth), bf16),
            jax.ShapeDtypeStruct((2 * down_rows, tp * width), bf16),
            jax.ShapeDtypeStruct((n_tok, width), bf16),
        ),
        in_specs=[vmem] * 4,
        out_specs=(anywhere, anywhere, anywhere, vmem),
        scratch_shapes=[
            pltpu.VMEM((tp, n_tok, width), bf16),
            pltpu.VMEM((n_tok, tp * width), bf16),
            pltpu.VMEM((fs, PIECES, units, depth), bf16),
            pltpu.VMEM((n_tok, units), bf16),
            pltpu.VMEM((tp, 2 * down_rows, width), bf16),
            pltpu.VMEM((3, n_tok, width), bf16),
            pltpu.VMEM((3, n_tok, width), bf16),
            dma((fs, PIECES)), dma((2, lines, PIECES)), dma((lines, PIECES)),
            dma((2, tp)), dma((2, 2, tp)), dma((tp,)), dma,
            dma((tp,)), dma((3,)), dma((3, tp)), dma((3, tp)), dma((4 + tp,)), dma((fs, PIECES)),
        ],
        compiler_params=pltpu.CompilerParams(
            collective_id=0, has_side_effects=True, vmem_limit_bytes=40 * 1024 * 1024
        ),
    )(tokens, gate_local.T, up_local.T, down_local)
    return gate.T, up.T, down_sampler, mixed


def plain(tokens, gate_local, up_local, down_local):
    gathered = lax.all_gather(tokens, "tp", axis=1, tiled=True)
    floated = gathered.astype(jnp.float32)
    normed = (
        floated * lax.rsqrt(jnp.mean(floated * floated, axis=-1, keepdims=True) + norm_eps)
    ).astype(jnp.bfloat16)
    gate_sampler = lax.all_gather(gate_local, "fs", axis=0, tiled=True)
    up_sampler = lax.all_gather(up_local, "fs", axis=0, tiled=True)
    gate = jnp.dot(normed, gate_sampler, preferred_element_type=jnp.float32)
    up = jnp.dot(normed, up_sampler, preferred_element_type=jnp.float32)
    hidden = (jax.nn.silu(gate) * up).astype(jnp.bfloat16)
    down_columns = lax.all_gather(down_local, "fs", axis=0, tiled=True)
    down_sampler = lax.all_to_all(down_columns, "tp", split_axis=0, concat_axis=1, tiled=True)
    mixed = jnp.dot(
        lax.all_gather(hidden, "tp", axis=1, tiled=True), down_columns, preferred_element_type=jnp.float32
    ).astype(jnp.bfloat16)
    return gate_sampler, up_sampler, down_sampler, mixed


def shards(fs, tp, tokens, norm_gain, gate_weight, up_weight, down_weight):
    gate_local = (norm_gain[:, None] * gate_weight).astype(jnp.bfloat16)
    up_local = (norm_gain[:, None] * up_weight).astype(jnp.bfloat16)
    down_local = down_weight.astype(jnp.bfloat16)
    aligned = (
        gate_local.shape[0] % 128 == 0
        and gate_local.shape[1] % 16 == 0
        and down_local.shape[0] % 16 == 0
        and down_local.shape[1] % 128 == 0
        and tokens.shape[0] % (128 * tp) == 0
    )
    if not (tp == 4 and fs == 2 * tp and aligned):
        return plain(tokens, gate_local, up_local, down_local)
    return fused(fs, tp, tokens, gate_local, up_local, down_local)


def solution(mesh):
    return jax.shard_map(
        functools.partial(shards, mesh.shape["fs"], mesh.shape["tp"]),
        mesh=mesh,
        in_specs=(P("fs", "tp"), P("fs"), P("fs", "tp"), P("fs", "tp"), P("fs", "tp")),
        out_specs=(P(None, "tp"), P(None, "tp"), P("tp", None), P("fs", "tp")),
        check_vma=False,
    )
```
